32 devices in a mesh: sp: 8 (over z, y), dp: 4 (over x, core).
Axes of the slice: x: 2, y: 2, z: 4, core: 2. Of those that a mesh axis runs over, the one named last changes fastest.
Arguments:
- queries: bfloat16 [4096, 6144], P(('dp', 'sp')), may hold values from -360 to 360
- latent: bfloat16 [4096, 1024], P(('dp', 'sp')), may hold values from -6 to 6
- rope_key: bfloat16 [4096, 64], P(('dp', 'sp')), may hold values from -6 to 6
- latent_gain: float32 [1024], replicated, may hold values from 0.1 to 1.9
- kv_weight: bfloat16 [1024, 8192], P(None, 'dp'), may hold values from -0.1875 to 0.1875
- gate: bfloat16 [4096, 4096], P(('dp', 'sp')), may hold values from -6 to 6
- out_gain: float32 [4096], replicated, may hold values from 0.1 to 1.9
Outputs:
- attended: bfloat16 [4096, 4096], P(('dp', 'sp'))
The draws below stay inside these ranges and needn't reach their ends.
All inputs are finite; a program needn't handle non-finite values.
Results may differ from the reference program's by a relative error of at most 0.007.
Values may be sent and summed in bfloat16 or wider, within the bound.
A program may use at most 128 MiB of HBM per device.

```python
import jax
import jax.numpy as jnp
from jax import lax

HEADS = 32
NOPE = 128
ROPE = 64
VDIM = 128
KV_RANK = 1024
SEQ_LEN = 1024
TOKENS = 4096


def draw_queries(key, part):
    values = jax.random.normal(key, (TOKENS, HEADS * (NOPE + ROPE)), jnp.float32)
    values = jnp.clip(values, -6.0, 6.0)
    return values.astype(jnp.bfloat16)


def steps_of(stream_key, extent, shards, low, largest):
    loudness = 1.0
    for dim, blocks in shards:
        steps = jax.random.uniform(jax.random.fold_in(jax.random.fold_in(stream_key, 6), dim), (blocks,), jnp.float32, low / len(shards), largest / len(shards))
        loudness = loudness * jnp.repeat(jnp.exp(steps), extent[dim] // blocks).reshape((-1,) + (1,) * (len(extent) - 1 - dim))
    return loudness


def bell_draw(own_key, shape, spread, limit, pieces=(), held_as=jnp.bfloat16):
    loudness = steps_of(own_key, shape, pieces, -0.22, 0.18) if pieces else 1.0
    values = jax.random.normal(own_key, shape, jnp.float32) * spread * loudness
    return jnp.minimum(jnp.maximum(values, -limit), limit).astype(held_as)


def setup_inputs(seed: int = 0) -> dict:
    streams_of = jax.random.split(jax.random.key(seed), 8)
    return {
        "queries": draw_queries(jax.random.fold_in(streams_of[7], 71), 0),
        "latent": bell_draw(streams_of[1], (TOKENS, KV_RANK), 1.0, 6.0, ((0, 32),)),
        "rope_key": bell_draw(streams_of[2], (TOKENS, ROPE), 1.0, 6.0, ((0, 32),)),
        "latent_gain": jnp.clip(1.0 + 0.18 * jax.random.normal(streams_of[3], (KV_RANK,), jnp.float32), 0.1, 1.9),
        "kv_weight": bell_draw(streams_of[4], (KV_RANK, HEADS * (NOPE + VDIM)), KV_RANK ** -0.5, 0.1875, ((1, 4),)),
        "gate": bell_draw(streams_of[5], (TOKENS, HEADS * VDIM), 1.0, 6.0, ((0, 32),)),
        "out_gain": jnp.clip(1.0 + 0.18 * jax.random.normal(streams_of[6], (HEADS * VDIM,), jnp.float32), 0.1, 1.9),
    }


EPS = 1e-06
THETA = 10000.0

def rotary(values, position):
    half_width = values.shape[-1] // 2
    inverse = THETA ** (-jnp.arange(half_width, dtype=jnp.float32) / half_width)
    angles = position.astype(jnp.float32)[:, None] * inverse[None, :]
    if values.ndim == 3:
        angles = angles[:, None, :]
    cosine = jnp.cos(angles)
    sine_part = jnp.sin(angles)
    front_half = values[..., :half_width].astype(jnp.float32)
    back_half = values[..., half_width:].astype(jnp.float32)
    turned = jnp.concatenate([front_half * cosine - back_half * sine_part, back_half * cosine + front_half * sine_part], axis=-1)
    return turned.astype(jnp.bfloat16)

def attend(query_block, keys_plain, keys_rotated, values):
    scores = jnp.einsum('qhd,khd->hqk', query_block[..., :NOPE].astype(jnp.float32), keys_plain.astype(jnp.float32))
    scores = scores + jnp.einsum('qhr,kr->hqk', query_block[..., NOPE:].astype(jnp.float32), keys_rotated.astype(jnp.float32))
    scores = scores * (NOPE + ROPE) ** (-0.5)
    row_max = lax.optimization_barrier(jnp.max(scores, axis=-1, keepdims=True))
    raised = jnp.exp(scores - row_max)
    weights = (raised / lax.optimization_barrier(jnp.sum(raised, axis=-1, keepdims=True))).astype(jnp.bfloat16)
    result = jnp.einsum('hqk,khd->qhd', weights.astype(jnp.float32), values.astype(jnp.float32))
    return result.astype(jnp.bfloat16)

def reference(queries, latent, rope_key, latent_gain, kv_weight, gate, out_gain):
    rows_all = queries.shape[0]
    position = jnp.arange(rows_all, dtype=jnp.int32) % SEQ_LEN
    widened = latent.astype(jnp.float32)
    normed = (widened * lax.rsqrt(lax.optimization_barrier(jnp.mean(widened * widened, axis=-1, keepdims=True)) + EPS) * latent_gain.astype(jnp.float32)).astype(jnp.bfloat16)
    keyval = jnp.dot(normed, kv_weight, preferred_element_type=jnp.float32).astype(jnp.bfloat16)
    head_queries = queries.reshape(rows_all, HEADS, NOPE + ROPE)
    head_queries = jnp.concatenate([head_queries[..., :NOPE], rotary(head_queries[..., NOPE:], position)], axis=-1)
    keys_rotated = rotary(rope_key, position)
    seq_count = rows_all // SEQ_LEN
    block_rows = min(512, SEQ_LEN)
    block_count = SEQ_LEN // block_rows

    def one_sequence(operands):
        query_seq, kv_seq, rope_seq = operands
        keys_plain = kv_seq[..., :NOPE]
        values = kv_seq[..., NOPE:]
        blocks = query_seq.reshape(block_count, block_rows, HEADS, NOPE + ROPE)
        result = lax.map(lambda piece_rows: attend(piece_rows, keys_plain, rope_seq, values), blocks)
        return result.reshape(SEQ_LEN, HEADS * VDIM)
    heads_out = lax.map(one_sequence, (head_queries.reshape(seq_count, SEQ_LEN, HEADS, NOPE + ROPE), keyval.reshape(seq_count, SEQ_LEN, HEADS, NOPE + VDIM), keys_rotated.reshape(seq_count, SEQ_LEN, ROPE)))
    heads_out = heads_out.reshape(rows_all, HEADS * VDIM)
    gated_rows = heads_out.astype(jnp.float32) * jax.nn.silu(gate.astype(jnp.float32))
    scale_rows = lax.rsqrt(lax.optimization_barrier(jnp.mean(gated_rows * gated_rows, axis=-1, keepdims=True)) + EPS)
    return (gated_rows * scale_rows * out_gain.astype(jnp.float32)).astype(jnp.bfloat16)
```

```python
import functools

import jax
import jax.numpy as jnp
import numpy as np
from jax import lax
from jax.experimental import pallas as pl
from jax.experimental.pallas import tpu as pltpu
from jax.sharding import PartitionSpec as P

HEADS = 32
NOPE = 128
ROPE = 64
VDIM = 128
QDIM = NOPE + ROPE
PAIR = 2 * QDIM
KDIM = 256

EPS = 1e-06
THETA = 10000.0
LOG2E = 1.4426950408889634

MESH = pl.DeviceIdType.MESH
DN_T = (((1,), (1,)), ((), ()))


def turn(x, cosine, sine, mask):
    partner = jnp.where(mask, pltpu.roll(x, 96, 1), pltpu.roll(x, 32, 1))
    return x * cosine + partner * sine


def kernel(
    n_s, n_d,
    q_ref, lat_ref, rk_ref, lgain_ref, w_ref, gate_ref, ogain_ref, ta_ref, tb_ref,
    out_ref,
    w_v, gate_v, silu, latz, rkz, latb, rkb, normed, rot, qb, kbuf, vbuf, rq, ob, orecv,
    w_sem, gate_sem, lat_send, lat_mid, rk_send, rk_mid, lat_fwd, rk_fwd, lat_recv, rk_recv,
    relay_lat, relay_rk, q_send, q_recv, o_send, o_recv,
):
    s, d = lax.axis_index("sp"), lax.axis_index("dp")
    rows = lat_ref.shape[0]
    heads = HEADS // n_d
    pairs = heads // 2
    half = n_d // 2
    n_z = n_s // half
    groups = n_z // 2
    x, core = d // 2, d % 2
    z, y = s // half, s % half
    zh, zl = z // 2, z % 2
    m = zl * half + y
    seq = 2 * ((y - zl + half) % half) + zl
    home_y = (x + core) % half
    home = core * half + home_y
    host_y = (x + zl) % half
    lead = core != zl
    partner = d + 1 - 2 * core

    def is_self(ts, td):
        return (ts == s) & (td == d)

    def send(src, dst, ssem, rsem, ts, td):
        same = is_self(ts, td)

        @pl.when(jnp.logical_not(same))
        def _():
            pltpu.make_async_remote_copy(
                src, dst, ssem, rsem, device_id={"sp": ts, "dp": td}, device_id_type=MESH
            ).start()

        @pl.when(same)
        def _():
            pltpu.make_async_copy(src, dst, rsem).start()

    def sent(src, dst, ssem, rsem, ts, td):
        same = is_self(ts, td)

        @pl.when(jnp.logical_not(same))
        def _():
            pltpu.make_async_remote_copy(
                src, dst, ssem, rsem, device_id={"sp": ts, "dp": td}, device_id_type=MESH
            ).wait_send()

    def arrived(dst, rsem):
        pltpu.make_async_copy(dst, dst, rsem).wait()

    w_copy = pltpu.make_async_copy(w_ref, w_v, w_sem)
    gate_copy = pltpu.make_async_copy(gate_ref, gate_v, gate_sem)
    w_copy.start()
    gate_copy.start()

    barrier = pltpu.get_barrier_semaphore()

    def greet(ts, td, when=None):
        there = jnp.logical_not(is_self(ts, td))
        if when is not None:
            there = there & when

        @pl.when(there)
        def _():
            pl.semaphore_signal(
                barrier, inc=1, device_id={"sp": ts, "dp": td}, device_id_type=MESH
            )

    for k in range(n_z):
        greet(k * half + y, 2 * x + zl, lead)
    for k in range(half):
        greet(z * half + k, 2 * (seq // 2) + core, lead)
    greet(s, partner, jnp.logical_not(lead))
    for k in range(n_d):
        greet(zh * n_d + k, seq)
        greet(zh * n_d + home, jnp.int32(k))

    def others(ts, td, count):
        return count - jnp.where(is_self(ts, td), 1, 0)

    meets = groups + others(zh * n_d + home, d, n_d) + others(s, seq, n_d)
    meets = meets + jnp.where(lead, 1 + others(z * half + host_y, d, half), 0)
    pl.semaphore_wait(barrier, meets)

    first_sends = []
    for k in range(groups):
        to = ((2 * k + core) * half + y, partner)
        first_sends.append((lat_ref, latz.at[z], lat_send.at[k], lat_mid.at[z], *to))
        first_sends.append((rk_ref, rkz.at[z], rk_send.at[k], rk_mid.at[z], *to))

    def forwards(from_z):
        slot = from_z * half + y
        for k in range(half):
            to = (z * half + host_y, 2 * k + core)
            yield latz.at[from_z], latb.at[slot], lat_fwd.at[from_z, k], lat_recv.at[slot], *to
            yield rkz.at[from_z], rkb.at[slot], rk_fwd.at[from_z, k], rk_recv.at[slot], *to

    def relays(slot):
        to = {"sp": s, "dp": partner}
        for buf, ssem, rsem in ((latb, relay_lat, lat_recv), (rkb, relay_rk, rk_recv)):
            yield pltpu.make_async_remote_copy(
                buf.at[slot], buf.at[slot], ssem.at[slot], rsem.at[slot],
                device_id=to, device_id_type=MESH,
            )

    query_sends = [
        (
            q_ref.at[:, pl.ds((t * pairs + p) * PAIR, PAIR)], qb.at[m, p],
            q_send.at[t, p], q_recv.at[m, p], zh * n_d + home, jnp.int32(t),
        )
        for p in range(pairs)
        for t in range(n_d)
    ]

    for args in first_sends:
        send(*args)

    @pl.when(jnp.logical_not(lead))
    def _():
        for args in query_sends:
            send(*args)

    gate_copy.wait()
    for c in range(0, HEADS * VDIM, 2 * VDIM):
        at = slice(c, c + 2 * VDIM)
        g = gate_v[:, at].astype(jnp.float32)
        silu[:, at] = g / (1.0 + jnp.exp(-g))

    lane = lax.broadcasted_iota(jnp.int32, (rows, 128), 1)
    mask = (lane % 64) < 32
    sign = jnp.where(mask, -1.0, 1.0).astype(jnp.float32)
    low = lax.broadcasted_iota(jnp.int32, (half * rows, 128), 1) < 64

    def tables(block):
        ca, sa = ta_ref[0], ta_ref[1]
        cb, sb = tb_ref[0, block], tb_ref[1, block]
        return ca * cb - sa * sb, (sa * cb + ca * sb) * sign

    def nearest(here, i, count):
        if count & (count - 1):
            return (here + i) % count
        out, bit = 0, 1
        while bit < count:
            out = out + bit * ((here // bit + i // bit) % 2)
            bit *= 2
        return out

    w_copy.wait()

    def forward_step(i):
        @pl.when(lead)
        def _():
            from_z = nearest(z, i, n_z)
            arrived(latz.at[from_z], lat_mid.at[from_z])
            arrived(rkz.at[from_z], rk_mid.at[from_z])
            for args in forwards(from_z):
                send(*args)

            @pl.when(i == n_z - 1)
            def _():
                for args in query_sends:
                    send(*args)

    def key_step(i, carry):
        @pl.when(i + 1 < n_z)
        def _():
            forward_step(i + 1)

        from_z = nearest(z, i, n_z)
        for k in range(half):
            slot = from_z * half + k
            here = slice(k * rows, (k + 1) * rows)
            arrived(latb.at[slot], lat_recv.at[slot])
            arrived(rkb.at[slot], rk_recv.at[slot])

            @pl.when(lead)
            def _():
                for copy in relays(slot):
                    copy.start()

            wide = latb[slot].astype(jnp.float32)
            scale = lax.rsqrt(jnp.mean(wide * wide, axis=-1, keepdims=True) + EPS)
            normed[here, :] = (wide * scale * lgain_ref[...]).astype(jnp.bfloat16)
            cosine, sine = tables(slot)
            raw = rkb[slot].astype(jnp.float32).T
            rot[here, :] = turn(
                jnp.concatenate([raw, jnp.zeros_like(raw)], axis=1), cosine, sine, mask
            )
        at = pl.ds(pl.multiple_of(from_z * half * rows, half * rows), half * rows)
        for h in range(heads):
            both = jnp.dot(
                normed[...], w_v[:, h * 256 : (h + 1) * 256], preferred_element_type=jnp.float32
            )
            plain = both[:, :NOPE]
            if h % 2 == 0:
                first, second = plain, rot[...]
            else:
                moved = pltpu.roll(plain, 64, 1)
                first = jnp.where(low, 0.0, moved)
                second = jnp.where(low, moved, pltpu.roll(rot[...], 64, 1))
            kbuf[h, at, :128] = first.astype(jnp.bfloat16)
            kbuf[h, at, 128:] = second.astype(jnp.bfloat16)
            vbuf[h, at, :VDIM] = both[:, NOPE:].astype(jnp.bfloat16)
            vbuf[h, at, VDIM:] = jnp.ones((half * rows, 128), jnp.bfloat16)
        return carry

    forward_step(jnp.int32(0))
    lax.fori_loop(0, n_z, key_step, 0)

    factor = LOG2E * QDIM ** -0.5

    def output_send(j, p):
        return (ob.at[j, p], orecv.at[d, p], o_send.at[j, p], o_recv.at[d, p], zh * n_d + j, seq)

    def query_step(i, carry):
        r, p = (i // pairs + m // 2) % half, i % pairs
        for part in range(2):
            slot = 2 * r + part
            arrived(qb.at[slot, p], q_recv.at[slot, p])
            cosine, sine = tables(zh * n_d + slot)
            cosine_high, sine_high = pltpu.roll(cosine, 64, 1), pltpu.roll(sine, 64, 1)
            here = slice(part * rows, (part + 1) * rows)
            rq[here, :128] = qb[slot, p, :, :128]
            v = qb[slot, p, :, 128:256].astype(jnp.float32)
            rq[here, 128:256] = turn(v, cosine, sine, mask).astype(jnp.bfloat16)
            v = qb[slot, p, :, 256:].astype(jnp.float32)
            rq[here, 256:] = turn(v, cosine_high, sine_high, mask).astype(jnp.bfloat16)
        for odd in range(2):
            h = 2 * p + odd
            scores = lax.dot_general(
                rq[:, odd * 128 : odd * 128 + KDIM], kbuf[h], DN_T, preferred_element_type=jnp.float32
            )
            top = jnp.max(scores, axis=-1, keepdims=True)
            raised = jnp.exp2((scores - top) * factor).astype(jnp.bfloat16)
            total = jnp.dot(raised, vbuf[h], preferred_element_type=jnp.float32)
            result = (total[:, :VDIM] / total[:, VDIM:]).astype(jnp.bfloat16)
            at = slice(odd * VDIM, (odd + 1) * VDIM)
            ob[2 * r, p, :, at] = result[:rows]
            ob[2 * r + 1, p, :, at] = result[rows:]
        send(*output_send(2 * r, p))
        send(*output_send(2 * r + 1, p))
        return carry

    lax.fori_loop(0, half * pairs, query_step, 0)

    square = jnp.zeros((rows, 1), jnp.float32)
    for p in range(pairs):
        for t in range(n_d):
            c = (t * pairs + p) * 2 * VDIM
            at = slice(c, c + 2 * VDIM)
            arrived(orecv.at[t, p], o_recv.at[t, p])
            gated = orecv[t, p].astype(jnp.float32) * silu[:, at]
            silu[:, at] = gated
            square = square + jnp.sum(gated * gated, axis=-1, keepdims=True)
    scale = lax.rsqrt(square / (HEADS * VDIM) + EPS)
    for c in range(0, HEADS * VDIM, 2 * VDIM):
        at = slice(c, c + 2 * VDIM)
        out_ref[:, at] = (silu[:, at] * scale * ogain_ref[:, at]).astype(jnp.bfloat16)

    for args in first_sends + query_sends:
        sent(*args)

    @pl.when(lead)
    def _():
        def forwarded(i, carry):
            for args in forwards(i):
                sent(*args)
            for k in range(half):
                for copy in relays(i * half + k):
                    copy.wait_send()
            return carry

        lax.fori_loop(0, n_z, forwarded, 0)

    def output_sent(i, carry):
        sent(*output_send(i // pairs, i % pairs))
        return carry

    lax.fori_loop(0, n_d * pairs, output_sent, 0)


def angle_tables(rows, n_s):
    half = ROPE // 2
    inverse = np.zeros(128)
    inverse[:ROPE] = np.tile(THETA ** (-np.arange(half) / half), 2)
    inner = np.arange(rows)[:, None] * inverse[None, :]
    outer = (np.arange(n_s) * rows)[:, None] * inverse[None, :]
    inner = np.stack([np.cos(inner), np.sin(inner)]).astype(np.float32)
    outer = np.stack([np.cos(outer), np.sin(outer)]).astype(np.float32)
    return jnp.asarray(inner), jnp.asarray(outer[:, :, None, :])


def per_device(n_s, n_d, queries, latent, rope_key, latent_gain, kv_weight, gate, out_gain):
    rows, rank = latent.shape
    heads = HEADS // n_d
    pairs = heads // 2
    seq = rows * n_s
    inner, outer = angle_tables(rows, n_s)
    bf = jnp.bfloat16
    dma = pltpu.SemaphoreType.DMA
    vmem = pl.BlockSpec(memory_space=pltpu.VMEM)
    hbm = pl.BlockSpec(memory_space=pl.ANY)
    half = n_d // 2
    n_z = n_s // half
    return pl.pallas_call(
        functools.partial(kernel, n_s, n_d),
        out_shape=jax.ShapeDtypeStruct(gate.shape, bf),
        in_specs=[hbm, vmem, vmem, vmem, hbm, hbm, vmem, vmem, vmem],
        out_specs=vmem,
        scratch_shapes=[
            pltpu.VMEM(kv_weight.shape, bf),
            pltpu.VMEM(gate.shape, bf),
            pltpu.VMEM(gate.shape, jnp.float32),
            pltpu.VMEM((n_z, rows, rank), bf),
            pltpu.VMEM((n_z, ROPE, rows), bf),
            pltpu.VMEM((n_s, rows, rank), bf),
            pltpu.VMEM((n_s, ROPE, rows), bf),
            pltpu.VMEM((half * rows, rank), bf),
            pltpu.VMEM((half * rows, 128), jnp.float32),
            pltpu.VMEM((n_d, pairs, rows, PAIR), bf),
            pltpu.VMEM((heads, seq, KDIM), bf),
            pltpu.VMEM((heads, seq, 2 * VDIM), bf),
            pltpu.VMEM((2 * rows, PAIR), bf),
            pltpu.VMEM((n_d, pairs, rows, 2 * VDIM), bf),
            pltpu.VMEM((n_d, pairs, rows, 2 * VDIM), bf),
            dma, dma,
            dma((n_z // 2,)), dma((n_z,)), dma((n_z // 2,)), dma((n_z,)),
            dma((n_z, half)), dma((n_z, half)),
            *[dma((n_s,))] * 4,
            *[dma((n_d, pairs))] * 4,
        ],
        compiler_params=pltpu.CompilerParams(
            collective_id=0, has_side_effects=True, vmem_limit_bytes=60 * 1024 * 1024
        ),
        name="latent_attention",
    )(
        queries, latent, rope_key.T, latent_gain[None, :], kv_weight, gate, out_gain[None, :],
        inner, outer,
    )


def solution(mesh):
    return jax.shard_map(
        functools.partial(per_device, mesh.shape["sp"], mesh.shape["dp"]),
        mesh=mesh,
        in_specs=(
            P(("dp", "sp"), None),
            P(("dp", "sp"), None),
            P(("dp", "sp"), None),
            P(),
            P(None, "dp"),
            P(("dp", "sp"), None),
            P(),
        ),
        out_specs=P(("dp", "sp"), None),
        check_vma=False,
    )
```

```python
import functools

import jax
import jax.numpy as jnp
import numpy as np
from jax import lax
from jax.experimental import pallas as pl
from jax.experimental.pallas import tpu as pltpu
from jax.sharding import PartitionSpec as P

HEADS = 32
NOPE = 128
ROPE = 64
VDIM = 128
QDIM = NOPE + ROPE
PAIR = 2 * QDIM
KDIM = 256

EPS = 1e-06
THETA = 10000.0
LOG2E = 1.4426950408889634
CHUNKS = 2
QUERIES_AT = (0, 2, 5, 8)

MESH = pl.DeviceIdType.MESH
DN_T = (((1,), (1,)), ((), ()))


def turn(x, cosine, sine, mask):
    partner = jnp.where(mask, pltpu.roll(x, 96, 1), pltpu.roll(x, 32, 1))
    return x * cosine + partner * sine


def kernel(
    n_s, n_d,
    q_ref, lat_ref, rk_ref, lgain_hbm, w_ref, gate_ref, ta_hbm, tb_hbm,
    gated_ref, scale_ref,
    w_v, gate_v, lgain_ref, ta_ref, tb_ref, latz, rkz, latb, rkb, normed, rot, qb, kbuf, vbuf, rq, ob, orecv,
    w_sem, gate_sem, small_sem, lat_send, lat_mid, rk_send, rk_mid, lat_fwd, rk_fwd, lat_recv, rk_recv,
    relay_lat, relay_rk, q_send, q_recv, o_send, o_recv,
):
    s, d = lax.axis_index("sp"), lax.axis_index("dp")
    rows = lat_ref.shape[0]
    heads = HEADS // n_d
    pairs = heads // 2
    half = n_d // 2
    n_z = n_s // half
    groups = n_z // 2
    x, core = d // 2, d % 2
    z, y = s // half, s % half
    zh, zl = z // 2, z % 2
    m = zl * half + y
    seq = 2 * ((y - zl + half) % half) + zl
    home_y = (x + core) % half
    home = core * half + home_y
    host_y = (x + zl) % half
    lead = core == zl
    partner = d + 1 - 2 * core
    chunk = rows // CHUNKS

    def is_self(ts, td):
        return (ts == s) & (td == d)

    def away(src, dst, ssem, rsem, ts, td):
        return pltpu.make_async_remote_copy(
            src, dst, ssem, rsem, device_id={"sp": ts, "dp": td}, device_id_type=MESH
        )

    def send(src, dst, ssem, rsem, ts, td):
        same = is_self(ts, td)

        @pl.when(jnp.logical_not(same))
        def _():
            pltpu.make_async_remote_copy(
                src, dst, ssem, rsem, device_id={"sp": ts, "dp": td}, device_id_type=MESH
            ).start()

        @pl.when(same)
        def _():
            pltpu.make_async_copy(src, dst, rsem).start()

    def sent(src, dst, ssem, rsem, ts, td):
        same = is_self(ts, td)

        @pl.when(jnp.logical_not(same))
        def _():
            pltpu.make_async_remote_copy(
                src, dst, ssem, rsem, device_id={"sp": ts, "dp": td}, device_id_type=MESH
            ).wait_send()

    def arrived(dst, rsem):
        pltpu.make_async_copy(dst, dst, rsem).wait()

    w_copy = pltpu.make_async_copy(w_ref, w_v, w_sem)
    gate_copy = pltpu.make_async_copy(gate_ref, gate_v, gate_sem)
    small_copies = [
        pltpu.make_async_copy(src, dst, small_sem.at[i])
        for i, (src, dst) in enumerate(
            ((lgain_hbm, lgain_ref), (ta_hbm, ta_ref), (tb_hbm, tb_ref))
        )
    ]
    gate_copy.start()
    w_copy.start()
    for copy in small_copies:
        copy.start()

    barrier = pltpu.get_barrier_semaphore()

    def greet(ts, td, when=None):
        there = jnp.logical_not(is_self(ts, td))
        if when is not None:
            there = there & when

        @pl.when(there)
        def _():
            pl.semaphore_signal(
                barrier, inc=1, device_id={"sp": ts, "dp": td}, device_id_type=MESH
            )

    for k in range(n_z):
        greet(k * half + y, d, lead)
    for k in range(half):
        greet(z * half + k, 2 * (seq // 2) + 1 - core, jnp.logical_not(lead))
    greet(s, partner, lead)
    for k in range(n_d):
        greet(zh * n_d + k, seq)
        greet(zh * n_d + home, jnp.int32(k))

    def others(ts, td, count):
        return count - jnp.where(is_self(ts, td), 1, 0)

    meets = groups + others(zh * n_d + home, d, n_d) + others(s, seq, n_d)
    meets = meets + jnp.where(lead, half - 1, 1)
    gate_copy.wait()
    for c in range(0, HEADS * VDIM, 2 * VDIM):
        at = slice(c, c + 2 * VDIM)
        g = gate_v[:, at].astype(jnp.float32)
        gated_ref[:, at] = g / (1.0 + jnp.exp(-g))
    pl.semaphore_wait(barrier, meets)

    first_sends = []
    for ch in range(CHUNKS):
        at = pl.ds(ch * chunk, chunk)
        for k in range(groups):
            to = ((2 * k + core) * half + y, d)
            first_sends.append(
                (lat_ref.at[at], latz.at[z, at], lat_send.at[k, ch], lat_mid.at[z, ch], *to)
            )
            if ch == 0:
                first_sends.append((rk_ref, rkz.at[z], rk_send.at[k], rk_mid.at[z], *to))

    def forwards(from_z, ch):
        slot = from_z * half + y
        at = pl.ds(ch * chunk, chunk)
        for k in range(half):
            to = (z * half + host_y, 2 * k + 1 - zl)
            yield (
                latz.at[from_z, at], latb.at[slot, at], lat_fwd.at[from_z, k, ch],
                lat_recv.at[slot], *to,
            )
            if ch == 0:
                yield rkz.at[from_z], rkb.at[slot], rk_fwd.at[from_z, k], rk_recv.at[slot], *to

    def relays(slot):
        to = {"sp": s, "dp": partner}
        for buf, ssem, rsem in ((latb, relay_lat, lat_recv), (rkb, relay_rk, rk_recv)):
            yield pltpu.make_async_remote_copy(
                buf.at[slot], buf.at[slot], ssem.at[slot], rsem.at[slot],
                device_id=to, device_id_type=MESH,
            )

    query_sends = [
        (
            q_ref.at[:, pl.ds((t * pairs + p) * PAIR, PAIR)], qb.at[m, p],
            q_send.at[t, p], q_recv.at[m, p], zh * n_d + home, jnp.int32(t),
        )
        for p in range(pairs)
        for t in range(n_d)
    ]

    for args in first_sends:
        send(*args)

    def query_part(p):
        for args in query_sends[p * n_d : (p + 1) * n_d]:
            send(*args)

    @pl.when(jnp.logical_not(lead))
    def _():
        for p in range(pairs):
            query_part(p)

    lane = lax.broadcasted_iota(jnp.int32, (rows, 128), 1)
    mask = (lane % 64) < 32
    sign = jnp.where(mask, -1.0, 1.0).astype(jnp.float32)
    low = lax.broadcasted_iota(jnp.int32, (half * rows, 128), 1) < 64

    def tables(block):
        ca, sa = ta_ref[0], ta_ref[1]
        cb, sb = tb_ref[0, block], tb_ref[1, block]
        return ca * cb - sa * sb, (sa * cb + ca * sb) * sign

    def nearest(here, i, count):
        if count & (count - 1):
            return (here + i) % count
        out, bit = 0, 1
        while bit < count:
            out = out + bit * ((here // bit + i // bit) % 2)
            bit *= 2
        return out

    w_copy.wait()
    for copy in small_copies:
        copy.wait()

    @pl.when(lead)
    def _():
        order = [(0, ch) for ch in range(CHUNKS)]
        order += [(i, ch) for ch in range(CHUNKS) for i in range(1, n_z)]
        for n, (i, ch) in enumerate(order):
            for p in range(pairs):
                if QUERIES_AT[p] == n:
                    query_part(p)
            from_z = nearest(z, i, n_z)
            at = pl.ds(ch * chunk, chunk)
            arrived(latz.at[from_z, at], lat_mid.at[from_z, ch])
            if ch == 0:
                arrived(rkz.at[from_z], rk_mid.at[from_z])
            for args in forwards(from_z, ch):
                away(*args).start()
        for p in range(pairs):
            if QUERIES_AT[p] >= len(order):
                query_part(p)

    def key_step(i, carry):
        from_z = nearest(z, i, n_z)
        for k in range(half):
            slot = from_z * half + k
            here = slice(k * rows, (k + 1) * rows)
            arrived(latb.at[slot], lat_recv.at[slot])
            arrived(rkb.at[slot], rk_recv.at[slot])

            @pl.when(jnp.logical_not(lead))
            def _():
                for copy in relays(slot):
                    copy.start()

            wide = latb[slot].astype(jnp.float32)
            scale = lax.rsqrt(jnp.mean(wide * wide, axis=-1, keepdims=True) + EPS)
            normed[here, :] = (wide * scale * lgain_ref[...]).astype(jnp.bfloat16)
            cosine, sine = tables(slot)
            raw = rkb[slot].astype(jnp.float32).T
            rot[here, :] = turn(
                jnp.concatenate([raw, jnp.zeros_like(raw)], axis=1), cosine, sine, mask
            )
        at = pl.ds(pl.multiple_of(from_z * half * rows, half * rows), half * rows)
        for h in range(heads):
            both = jnp.dot(
                normed[...], w_v[:, h * 256 : (h + 1) * 256], preferred_element_type=jnp.float32
            )
            plain = both[:, :NOPE]
            if h % 2 == 0:
                first, second = plain, rot[...]
            else:
                moved = pltpu.roll(plain, 64, 1)
                first = jnp.where(low, 0.0, moved)
                second = jnp.where(low, moved, pltpu.roll(rot[...], 64, 1))
            kbuf[h, at, :128] = first.astype(jnp.bfloat16)
            kbuf[h, at, 128:] = second.astype(jnp.bfloat16)
            vbuf[h, at, :VDIM] = both[:, NOPE:].astype(jnp.bfloat16)
            vbuf[h, at, VDIM:] = jnp.ones((half * rows, 128), jnp.bfloat16)
        return carry

    lax.fori_loop(0, n_z, key_step, 0)

    factor = LOG2E * QDIM ** -0.5

    def output_send(j, p):
        return (ob.at[j, p], orecv.at[d, p], o_send.at[j, p], o_recv.at[d, p], zh * n_d + j, seq)

    def query_step(i, carry):
        r, p = (i % half + m // 2) % half, i // half
        for part in range(2):
            slot = 2 * r + part
            arrived(qb.at[slot, p], q_recv.at[slot, p])
            cosine, sine = tables(zh * n_d + slot)
            cosine_high, sine_high = pltpu.roll(cosine, 64, 1), pltpu.roll(sine, 64, 1)
            here = slice(part * rows, (part + 1) * rows)
            rq[here, :128] = qb[slot, p, :, :128]
            v = qb[slot, p, :, 128:256].astype(jnp.float32)
            rq[here, 128:256] = turn(v, cosine, sine, mask).astype(jnp.bfloat16)
            v = qb[slot, p, :, 256:].astype(jnp.float32)
            rq[here, 256:] = turn(v, cosine_high, sine_high, mask).astype(jnp.bfloat16)
        for odd in range(2):
            h = 2 * p + odd
            scores = lax.dot_general(
                rq[:, odd * 128 : odd * 128 + KDIM], kbuf[h], DN_T, preferred_element_type=jnp.float32
            )
            top = jnp.max(scores, axis=-1, keepdims=True)
            raised = jnp.exp2((scores - top) * factor).astype(jnp.bfloat16)
            total = jnp.dot(raised, vbuf[h], preferred_element_type=jnp.float32)
            result = (total[:, :VDIM] / total[:, VDIM:]).astype(jnp.bfloat16)
            at = slice(odd * VDIM, (odd + 1) * VDIM)
            ob[2 * r, p, :, at] = result[:rows]
            ob[2 * r + 1, p, :, at] = result[rows:]
        send(*output_send(2 * r, p))
        send(*output_send(2 * r + 1, p))
        return carry

    lax.fori_loop(0, half * pairs, query_step, 0)

    square = jnp.zeros((rows, 1), jnp.float32)
    for p in range(pairs):
        for t in range(n_d):
            c = (t * pairs + p) * 2 * VDIM
            at = slice(c, c + 2 * VDIM)
            arrived(orecv.at[t, p], o_recv.at[t, p])
            gated = orecv[t, p].astype(jnp.float32) * gated_ref[:, at]
            gated_ref[:, at] = gated
            square = square + jnp.sum(gated * gated, axis=-1, keepdims=True)
    scale = lax.rsqrt(square / (HEADS * VDIM) + EPS)
    scale_ref[...] = jnp.broadcast_to(scale, scale_ref.shape)

    for args in first_sends + query_sends:
        sent(*args)

    @pl.when(lead)
    def _():
        for i in range(n_z):
            for ch in range(CHUNKS):
                for args in forwards(i, ch):
                    away(*args).wait_send()

    @pl.when(jnp.logical_not(lead))
    def _():
        def relayed(i, carry):
            for copy in relays(i):
                copy.wait_send()
            return carry

        lax.fori_loop(0, n_s, relayed, 0)

    def output_sent(i, carry):
        sent(*output_send(i // pairs, i % pairs))
        return carry

    lax.fori_loop(0, n_d * pairs, output_sent, 0)


def angle_tables(rows, n_s):
    half = ROPE // 2
    inverse = np.zeros(128)
    inverse[:ROPE] = np.tile(THETA ** (-np.arange(half) / half), 2)
    inner = np.arange(rows)[:, None] * inverse[None, :]
    outer = (np.arange(n_s) * rows)[:, None] * inverse[None, :]
    inner = np.stack([np.cos(inner), np.sin(inner)]).astype(np.float32)
    outer = np.stack([np.cos(outer), np.sin(outer)]).astype(np.float32)
    return jnp.asarray(inner), jnp.asarray(outer[:, :, None, :])


def per_device(n_s, n_d, queries, latent, rope_key, latent_gain, kv_weight, gate, out_gain):
    rows, rank = latent.shape
    heads = HEADS // n_d
    pairs = heads // 2
    seq = rows * n_s
    inner, outer = angle_tables(rows, n_s)
    bf = jnp.bfloat16
    dma = pltpu.SemaphoreType.DMA
    vmem = pl.BlockSpec(memory_space=pltpu.VMEM)
    hbm = pl.BlockSpec(memory_space=pl.ANY)
    half = n_d // 2
    n_z = n_s // half
    gated, scale = pl.pallas_call(
        functools.partial(kernel, n_s, n_d),
        out_shape=(
            pltpu.VMEM(gate.shape, jnp.float32),
            pltpu.VMEM((rows, 128), jnp.float32),
        ),
        in_specs=[hbm] * 8,
        out_specs=(vmem, vmem),
        scratch_shapes=[
            pltpu.VMEM(kv_weight.shape, bf),
            pltpu.VMEM(gate.shape, bf),
            pltpu.VMEM((1, rank), jnp.float32),
            pltpu.VMEM(inner.shape, jnp.float32),
            pltpu.VMEM(outer.shape, jnp.float32),
            pltpu.VMEM((n_z, rows, rank), bf),
            pltpu.VMEM((n_z, ROPE, rows), bf),
            pltpu.VMEM((n_s, rows, rank), bf),
            pltpu.VMEM((n_s, ROPE, rows), bf),
            pltpu.VMEM((half * rows, rank), bf),
            pltpu.VMEM((half * rows, 128), jnp.float32),
            pltpu.VMEM((n_d, pairs, rows, PAIR), bf),
            pltpu.VMEM((heads, seq, KDIM), bf),
            pltpu.VMEM((heads, seq, 2 * VDIM), bf),
            pltpu.VMEM((2 * rows, PAIR), bf),
            pltpu.VMEM((n_d, pairs, rows, 2 * VDIM), bf),
            pltpu.VMEM((n_d, pairs, rows, 2 * VDIM), bf),
            dma, dma, dma((3,)),
            dma((n_z // 2, CHUNKS)), dma((n_z, CHUNKS)), dma((n_z // 2,)), dma((n_z,)),
            dma((n_z, half, CHUNKS)), dma((n_z, half)),
            *[dma((n_s,))] * 4,
            *[dma((n_d, pairs))] * 4,
        ],
        compiler_params=pltpu.CompilerParams(
            collective_id=0, has_side_effects=True, vmem_limit_bytes=60 * 1024 * 1024
        ),
        name="latent_attention",
    )(
        queries, latent, rope_key.T, latent_gain[None, :], kv_weight, gate, inner, outer,
    )
    return (gated * scale[:, :1] * out_gain[None, :]).astype(bf)


def solution(mesh):
    return jax.shard_map(
        functools.partial(per_device, mesh.shape["sp"], mesh.shape["dp"]),
        mesh=mesh,
        in_specs=(
            P(("dp", "sp"), None),
            P(("dp", "sp"), None),
            P(("dp", "sp"), None),
            P(),
            P(None, "dp"),
            P(("dp", "sp"), None),
            P(),
        ),
        out_specs=P(("dp", "sp"), None),
        check_vma=False,
    )
```

```python
import functools

import jax
import jax.numpy as jnp
import numpy as np
from jax import lax
from jax.experimental import pallas as pl
from jax.experimental.pallas import tpu as pltpu
from jax.sharding import PartitionSpec as P

HEADS = 32
NOPE = 128
ROPE = 64
VDIM = 128
QDIM = NOPE + ROPE
PAIR = 2 * QDIM
KDIM = 256

EPS = 1e-06
THETA = 10000.0
LOG2E = 1.4426950408889634
CHUNKS = 2
QUERIES_AT = (0, 2, 4, 8)
CROSSING_AT = (0, 1, 2, 3)
TARGETS = (0, 1, 2, 3)

MESH = pl.DeviceIdType.MESH
DN_T = (((1,), (1,)), ((), ()))


def turn(x, cosine, sine, mask):
    partner = jnp.where(mask, pltpu.roll(x, 96, 1), pltpu.roll(x, 32, 1))
    return x * cosine + partner * sine


def kernel(
    n_s, n_d,
    q_ref, lat_ref, rk_ref, lgain_hbm, w_ref, gate_ref, ta_hbm, tb_hbm,
    gated_ref, scale_ref,
    w_v, gate_v, lgain_ref, ta_ref, tb_ref, latz, rkz, latb, rkb, normed, rot, qb, kbuf, vbuf, rq, ob, orecv,
    w_sem, gate_sem, small_sem, lat_send, lat_mid, rk_send, rk_mid, lat_fwd, rk_fwd, lat_recv, rk_recv,
    relay_lat, relay_rk, q_send, q_recv, o_send, o_recv,
):
    s, d = lax.axis_index("sp"), lax.axis_index("dp")
    rows = lat_ref.shape[0]
    heads = HEADS // n_d
    pairs = heads // 2
    half = n_d // 2
    n_z = n_s // half
    groups = n_z // 2
    x, core = d // 2, d % 2
    z, y = s // half, s % half
    zh, zl = z // 2, z % 2
    m = zl * half + y
    seq = 2 * ((y - zl + half) % half) + zl
    home_y = (x + core) % half
    home = core * half + home_y
    host_y = (x + zl) % half
    lead = core == zl
    partner = d + 1 - 2 * core
    chunk = rows // CHUNKS

    def is_self(ts, td):
        return (ts == s) & (td == d)

    def away(src, dst, ssem, rsem, ts, td):
        return pltpu.make_async_remote_copy(
            src, dst, ssem, rsem, device_id={"sp": ts, "dp": td}, device_id_type=MESH
        )

    def send(src, dst, ssem, rsem, ts, td):
        same = is_self(ts, td)

        @pl.when(jnp.logical_not(same))
        def _():
            pltpu.make_async_remote_copy(
                src, dst, ssem, rsem, device_id={"sp": ts, "dp": td}, device_id_type=MESH
            ).start()

        @pl.when(same)
        def _():
            pltpu.make_async_copy(src, dst, rsem).start()

    def sent(src, dst, ssem, rsem, ts, td):
        same = is_self(ts, td)

        @pl.when(jnp.logical_not(same))
        def _():
            pltpu.make_async_remote_copy(
                src, dst, ssem, rsem, device_id={"sp": ts, "dp": td}, device_id_type=MESH
            ).wait_send()

    def arrived(dst, rsem):
        pltpu.make_async_copy(dst, dst, rsem).wait()

    w_copy = pltpu.make_async_copy(w_ref, w_v, w_sem)
    gate_copy = pltpu.make_async_copy(gate_ref, gate_v, gate_sem)
    small_copies = [
        pltpu.make_async_copy(src, dst, small_sem.at[i])
        for i, (src, dst) in enumerate(
            ((lgain_hbm, lgain_ref), (ta_hbm, ta_ref), (tb_hbm, tb_ref))
        )
    ]
    gate_copy.start()
    w_copy.start()
    for copy in small_copies:
        copy.start()

    barrier = pltpu.get_barrier_semaphore()

    def greet(ts, td, when=None):
        there = jnp.logical_not(is_self(ts, td))
        if when is not None:
            there = there & when

        @pl.when(there)
        def _():
            pl.semaphore_signal(
                barrier, inc=1, device_id={"sp": ts, "dp": td}, device_id_type=MESH
            )

    for k in range(n_z):
        greet(k * half + y, d, lead)
    for k in range(half):
        greet(z * half + k, 2 * (seq // 2) + 1 - core, jnp.logical_not(lead))
    greet(s, partner, lead)
    for k in range(n_d):
        greet(zh * n_d + k, seq)
        greet(zh * n_d + home, jnp.int32(k))

    def others(ts, td, count):
        return count - jnp.where(is_self(ts, td), 1, 0)

    meets = groups + others(zh * n_d + home, d, n_d) + others(s, seq, n_d)
    meets = meets + jnp.where(lead, half - 1, 1)
    gate_copy.wait()
    for c in range(0, HEADS * VDIM, 2 * VDIM):
        at = slice(c, c + 2 * VDIM)
        g = gate_v[:, at].astype(jnp.float32)
        gated_ref[:, at] = g / (1.0 + jnp.exp(-g))
    pl.semaphore_wait(barrier, meets)

    first_sends = []
    for ch in range(CHUNKS):
        at = pl.ds(ch * chunk, chunk)
        for k in range(groups):
            to = ((2 * k + core) * half + y, d)
            first_sends.append(
                (lat_ref.at[at], latz.at[z, at], lat_send.at[k, ch], lat_mid.at[z, ch], *to)
            )
            if ch == 0:
                first_sends.append((rk_ref, rkz.at[z], rk_send.at[k], rk_mid.at[z], *to))

    def forwards(from_z, ch):
        slot = from_z * half + y
        at = pl.ds(ch * chunk, chunk)
        for k in range(half):
            to = (z * half + host_y, 2 * k + 1 - zl)
            yield (
                latz.at[from_z, at], latb.at[slot, at], lat_fwd.at[from_z, k, ch],
                lat_recv.at[slot], *to,
            )
            if ch == 0:
                yield rkz.at[from_z], rkb.at[slot], rk_fwd.at[from_z, k], rk_recv.at[slot], *to

    def relays(slot):
        to = {"sp": s, "dp": partner}
        for buf, ssem, rsem in ((latb, relay_lat, lat_recv), (rkb, relay_rk, rk_recv)):
            yield pltpu.make_async_remote_copy(
                buf.at[slot], buf.at[slot], ssem.at[slot], rsem.at[slot],
                device_id=to, device_id_type=MESH,
            )

    def query_sends_of(p):
        for t in TARGETS:
            t = ((x + t // 2) % half) * 2 + (core + t % 2) % 2
            yield (
                q_ref.at[:, pl.ds(pl.multiple_of((t * pairs + p) * PAIR, PAIR), PAIR)],
                qb.at[m, p], q_send.at[t, p], q_recv.at[m, p], zh * n_d + home, t,
            )

    query_sends = [args for p in range(pairs) for args in query_sends_of(p)]

    for args in first_sends:
        send(*args)

    def query_part(p):
        for args in query_sends[p * n_d : (p + 1) * n_d]:
            send(*args)

    @pl.when(jnp.logical_not(lead))
    def _():
        for p in range(pairs):
            if CROSSING_AT[p % len(CROSSING_AT)] == 0:
                query_part(p)

    lane = lax.broadcasted_iota(jnp.int32, (rows, 128), 1)
    mask = (lane % 64) < 32
    sign = jnp.where(mask, -1.0, 1.0).astype(jnp.float32)
    low = lax.broadcasted_iota(jnp.int32, (half * rows, 128), 1) < 64

    def tables(block):
        ca, sa = ta_ref[0], ta_ref[1]
        cb, sb = tb_ref[0, block], tb_ref[1, block]
        return ca * cb - sa * sb, (sa * cb + ca * sb) * sign

    def nearest(here, i, count):
        if count & (count - 1):
            return (here + i) % count
        out, bit = 0, 1
        while bit < count:
            out = out + bit * ((here // bit + i // bit) % 2)
            bit *= 2
        return out

    w_copy.wait()
    for copy in small_copies:
        copy.wait()

    stages = [[(i, ch) for i in range(2) for ch in range(CHUNKS)]]
    stages += [[(i, ch) for i in range(2, n_z)] for ch in range(CHUNKS)]
    starts = [sum(map(len, stages[:k])) for k in range(len(stages) + 1)]

    def forward_stage(k):
        for n, (i, ch) in enumerate(stages[k], starts[k]):
            for p in range(pairs):
                if QUERIES_AT[p % len(QUERIES_AT)] == n:
                    query_part(p)
            from_z = nearest(z, i, n_z)
            at = pl.ds(ch * chunk, chunk)
            arrived(latz.at[from_z, at], lat_mid.at[from_z, ch])
            if ch == 0:
                arrived(rkz.at[from_z], rk_mid.at[from_z])
            for args in forwards(from_z, ch):
                away(*args).start()
        if k == len(stages) - 1:
            for p in range(pairs):
                if QUERIES_AT[p % len(QUERIES_AT)] >= starts[-1]:
                    query_part(p)

    def key_step(i, carry):
        for k in range(len(stages)):

            @pl.when(lead & (i == k))
            def _():
                forward_stage(k)

        from_z = nearest(z, i, n_z)
        for k in range(half):
            slot = from_z * half + k
            here = slice(k * rows, (k + 1) * rows)
            arrived(latb.at[slot], lat_recv.at[slot])
            arrived(rkb.at[slot], rk_recv.at[slot])

            @pl.when(jnp.logical_not(lead))
            def _():
                for copy in relays(slot):
                    copy.start()

            wide = latb[slot].astype(jnp.float32)
            scale = lax.rsqrt(jnp.mean(wide * wide, axis=-1, keepdims=True) + EPS)
            normed[here, :] = (wide * scale * lgain_ref[...]).astype(jnp.bfloat16)
            cosine, sine = tables(slot)
            raw = rkb[slot].astype(jnp.float32).T
            rot[here, :] = turn(
                jnp.concatenate([raw, jnp.zeros_like(raw)], axis=1), cosine, sine, mask
            )
        at = pl.ds(pl.multiple_of(from_z * half * rows, half * rows), half * rows)
        for h in range(heads):
            both = jnp.dot(
                normed[...], w_v[:, h * 256 : (h + 1) * 256], preferred_element_type=jnp.float32
            )
            plain = both[:, :NOPE]
            if h % 2 == 0:
                first, second = plain, rot[...]
            else:
                moved = pltpu.roll(plain, 64, 1)
                first = jnp.where(low, 0.0, moved)
                second = jnp.where(low, moved, pltpu.roll(rot[...], 64, 1))
            kbuf[h, at, :128] = first.astype(jnp.bfloat16)
            kbuf[h, at, 128:] = second.astype(jnp.bfloat16)
            vbuf[h, at, :VDIM] = both[:, NOPE:].astype(jnp.bfloat16)
            vbuf[h, at, VDIM:] = jnp.ones((half * rows, 128), jnp.bfloat16)
        for step in sorted(set(CROSSING_AT) - {0}):

            @pl.when(jnp.logical_not(lead) & (i + 1 == step))
            def _():
                for p in range(pairs):
                    if CROSSING_AT[p % len(CROSSING_AT)] == step:
                        query_part(p)
        return carry

    lax.fori_loop(0, n_z, key_step, 0)

    factor = LOG2E * QDIM ** -0.5

    def output_send(j, p):
        return (ob.at[j, p], orecv.at[d, p], o_send.at[j, p], o_recv.at[d, p], zh * n_d + j, seq)

    def query_step(i, carry):
        r, p = (i % half + m // 2) % half, i // half
        for part in range(2):
            slot = 2 * r + part
            arrived(qb.at[slot, p], q_recv.at[slot, p])
            cosine, sine = tables(zh * n_d + slot)
            cosine_high, sine_high = pltpu.roll(cosine, 64, 1), pltpu.roll(sine, 64, 1)
            here = slice(part * rows, (part + 1) * rows)
            rq[here, :128] = qb[slot, p, :, :128]
            v = qb[slot, p, :, 128:256].astype(jnp.float32)
            rq[here, 128:256] = turn(v, cosine, sine, mask).astype(jnp.bfloat16)
            v = qb[slot, p, :, 256:].astype(jnp.float32)
            rq[here, 256:] = turn(v, cosine_high, sine_high, mask).astype(jnp.bfloat16)
        for odd in range(2):
            h = 2 * p + odd
            scores = lax.dot_general(
                rq[:, odd * 128 : odd * 128 + KDIM], kbuf[h], DN_T, preferred_element_type=jnp.float32
            )
            top = jnp.max(scores, axis=-1, keepdims=True)
            raised = jnp.exp2((scores - top) * factor).astype(jnp.bfloat16)
            total = jnp.dot(raised, vbuf[h], preferred_element_type=jnp.float32)
            result = (total[:, :VDIM] / total[:, VDIM:]).astype(jnp.bfloat16)
            at = slice(odd * VDIM, (odd + 1) * VDIM)
            ob[2 * r, p, :, at] = result[:rows]
            ob[2 * r + 1, p, :, at] = result[rows:]
        send(*output_send(2 * r, p))
        send(*output_send(2 * r + 1, p))
        return carry

    lax.fori_loop(0, half * pairs, query_step, 0)

    square = jnp.zeros((rows, 1), jnp.float32)
    for p in range(pairs):
        for t in range(n_d):
            c = (t * pairs + p) * 2 * VDIM
            at = slice(c, c + 2 * VDIM)
            arrived(orecv.at[t, p], o_recv.at[t, p])
            gated = orecv[t, p].astype(jnp.float32) * gated_ref[:, at]
            gated_ref[:, at] = gated
            square = square + jnp.sum(gated * gated, axis=-1, keepdims=True)
    scale = lax.rsqrt(square / (HEADS * VDIM) + EPS)
    scale_ref[...] = jnp.broadcast_to(scale, scale_ref.shape)

    for args in first_sends + query_sends:
        sent(*args)

    @pl.when(lead)
    def _():
        for i in range(n_z):
            for ch in range(CHUNKS):
                for args in forwards(i, ch):
                    away(*args).wait_send()

    @pl.when(jnp.logical_not(lead))
    def _():
        def relayed(i, carry):
            for copy in relays(i):
                copy.wait_send()
            return carry

        lax.fori_loop(0, n_s, relayed, 0)

    def output_sent(i, carry):
        sent(*output_send(i // pairs, i % pairs))
        return carry

    lax.fori_loop(0, n_d * pairs, output_sent, 0)


def angle_tables(rows, n_s):
    half = ROPE // 2
    inverse = np.zeros(128)
    inverse[:ROPE] = np.tile(THETA ** (-np.arange(half) / half), 2)
    inner = np.arange(rows)[:, None] * inverse[None, :]
    outer = (np.arange(n_s) * rows)[:, None] * inverse[None, :]
    inner = np.stack([np.cos(inner), np.sin(inner)]).astype(np.float32)
    outer = np.stack([np.cos(outer), np.sin(outer)]).astype(np.float32)
    return jnp.asarray(inner), jnp.asarray(outer[:, :, None, :])


def per_device(n_s, n_d, queries, latent, rope_key, latent_gain, kv_weight, gate, out_gain):
    rows, rank = latent.shape
    heads = HEADS // n_d
    pairs = heads // 2
    seq = rows * n_s
    inner, outer = angle_tables(rows, n_s)
    bf = jnp.bfloat16
    dma = pltpu.SemaphoreType.DMA
    vmem = pl.BlockSpec(memory_space=pltpu.VMEM)
    hbm = pl.BlockSpec(memory_space=pl.ANY)
    half = n_d // 2
    n_z = n_s // half
    gated, scale = pl.pallas_call(
        functools.partial(kernel, n_s, n_d),
        out_shape=(
            pltpu.VMEM(gate.shape, jnp.float32),
            pltpu.VMEM((rows, 128), jnp.float32),
        ),
        in_specs=[hbm] * 8,
        out_specs=(vmem, vmem),
        scratch_shapes=[
            pltpu.VMEM(kv_weight.shape, bf),
            pltpu.VMEM(gate.shape, bf),
            pltpu.VMEM((1, rank), jnp.float32),
            pltpu.VMEM(inner.shape, jnp.float32),
            pltpu.VMEM(outer.shape, jnp.float32),
            pltpu.VMEM((n_z, rows, rank), bf),
            pltpu.VMEM((n_z, ROPE, rows), bf),
            pltpu.VMEM((n_s, rows, rank), bf),
            pltpu.VMEM((n_s, ROPE, rows), bf),
            pltpu.VMEM((half * rows, rank), bf),
            pltpu.VMEM((half * rows, 128), jnp.float32),
            pltpu.VMEM((n_d, pairs, rows, PAIR), bf),
            pltpu.VMEM((heads, seq, KDIM), bf),
            pltpu.VMEM((heads, seq, 2 * VDIM), bf),
            pltpu.VMEM((2 * rows, PAIR), bf),
            pltpu.VMEM((n_d, pairs, rows, 2 * VDIM), bf),
            pltpu.VMEM((n_d, pairs, rows, 2 * VDIM), bf),
            dma, dma, dma((3,)),
            dma((n_z // 2, CHUNKS)), dma((n_z, CHUNKS)), dma((n_z // 2,)), dma((n_z,)),
            dma((n_z, half, CHUNKS)), dma((n_z, half)),
            *[dma((n_s,))] * 4,
            *[dma((n_d, pairs))] * 4,
        ],
        compiler_params=pltpu.CompilerParams(
            collective_id=0, has_side_effects=True, vmem_limit_bytes=60 * 1024 * 1024
        ),
        name="latent_attention",
    )(
        queries, latent, rope_key.T, latent_gain[None, :], kv_weight, gate, inner, outer,
    )
    return (gated * scale[:, :1] * out_gain[None, :]).astype(bf)


def solution(mesh):
    return jax.shard_map(
        functools.partial(per_device, mesh.shape["sp"], mesh.shape["dp"]),
        mesh=mesh,
        in_specs=(
            P(("dp", "sp"), None),
            P(("dp", "sp"), None),
            P(("dp", "sp"), None),
            P(),
            P(None, "dp"),
            P(("dp", "sp"), None),
            P(),
        ),
        out_specs=P(("dp", "sp"), None),
        check_vma=False,
    )
```

```python
import functools

import jax
import jax.numpy as jnp
import numpy as np
from jax import lax
from jax.experimental import pallas as pl
from jax.experimental.pallas import tpu as pltpu
from jax.sharding import PartitionSpec as P

HEADS = 32
NOPE = 128
ROPE = 64
VDIM = 128
QDIM = NOPE + ROPE
PAIR = 2 * QDIM
KDIM = 256

EPS = 1e-06
THETA = 10000.0
LOG2E = 1.4426950408889634
CHUNKS = 2
QUERIES_AT = (0, 2, 4, 8)
CROSSING_AT = (0, 0, 2, 3)
TARGETS = (0, 1, 2, 3)

MESH = pl.DeviceIdType.MESH
DN_T = (((1,), (1,)), ((), ()))


def turn(x, cosine, sine, mask):
    partner = jnp.where(mask, pltpu.roll(x, 96, 1), pltpu.roll(x, 32, 1))
    return x * cosine + partner * sine


def kernel(
    n_s, n_d,
    q_ref, lat_hbm, rk_hbm, lgain_hbm, w_ref, gate_ref, ta_hbm, tb_hbm,
    gated_ref, scale_ref,
    w_v, gate_v, lat_ref, rk_ref, lgain_ref, ta_ref, tb_ref, latz, rkz, latb, rkb, normed, rot, qb, kbuf, vbuf, rq, ob, orecv,
    w_sem, gate_sem, small_sem, lat_send, lat_mid, rk_send, rk_mid, lat_fwd, rk_fwd, lat_recv, rk_recv,
    relay_lat, relay_rk, q_send, q_recv, o_send, o_recv,
):
    s, d = lax.axis_index("sp"), lax.axis_index("dp")
    rows = lat_ref.shape[0]
    heads = HEADS // n_d
    pairs = heads // 2
    half = n_d // 2
    n_z = n_s // half
    groups = n_z // 2
    x, core = d // 2, d % 2
    z, y = s // half, s % half
    zh, zl = z // 2, z % 2
    m = zl * half + y
    seq = 2 * ((y - zl + half) % half) + zl
    home_y = (x + core) % half
    home = core * half + home_y
    host_y = (x + zl) % half
    lead = core == zl
    partner = d + 1 - 2 * core
    chunk = rows // CHUNKS

    def is_self(ts, td):
        return (ts == s) & (td == d)

    def away(src, dst, ssem, rsem, ts, td):
        return pltpu.make_async_remote_copy(
            src, dst, ssem, rsem, device_id={"sp": ts, "dp": td}, device_id_type=MESH
        )

    def send(src, dst, ssem, rsem, ts, td):
        same = is_self(ts, td)

        @pl.when(jnp.logical_not(same))
        def _():
            pltpu.make_async_remote_copy(
                src, dst, ssem, rsem, device_id={"sp": ts, "dp": td}, device_id_type=MESH
            ).start()

        @pl.when(same)
        def _():
            pltpu.make_async_copy(src, dst, rsem).start()

    def sent(src, dst, ssem, rsem, ts, td):
        same = is_self(ts, td)

        @pl.when(jnp.logical_not(same))
        def _():
            pltpu.make_async_remote_copy(
                src, dst, ssem, rsem, device_id={"sp": ts, "dp": td}, device_id_type=MESH
            ).wait_send()

    def arrived(dst, rsem):
        pltpu.make_async_copy(dst, dst, rsem).wait()

    w_copy = pltpu.make_async_copy(w_ref, w_v, w_sem)
    gate_copy = pltpu.make_async_copy(gate_ref, gate_v, gate_sem)
    small_copies = [
        pltpu.make_async_copy(src, dst, small_sem.at[i])
        for i, (src, dst) in enumerate(
            (
                (lat_hbm, lat_ref), (rk_hbm, rk_ref), (lgain_hbm, lgain_ref),
                (ta_hbm, ta_ref), (tb_hbm, tb_ref),
            )
        )
    ]
    gate_copy.start()
    for copy in small_copies:
        copy.start()
    w_copy.start()

    barrier = pltpu.get_barrier_semaphore()

    def greet(ts, td, when=None):
        there = jnp.logical_not(is_self(ts, td))
        if when is not None:
            there = there & when

        @pl.when(there)
        def _():
            pl.semaphore_signal(
                barrier, inc=1, device_id={"sp": ts, "dp": td}, device_id_type=MESH
            )

    for k in range(n_z):
        greet(k * half + y, d, lead)
    for k in range(half):
        greet(z * half + k, 2 * (seq // 2) + 1 - core, jnp.logical_not(lead))
    greet(s, partner, lead)
    for k in range(n_d):
        greet(zh * n_d + k, seq)
        greet(zh * n_d + home, jnp.int32(k))

    def others(ts, td, count):
        return count - jnp.where(is_self(ts, td), 1, 0)

    meets = groups + others(zh * n_d + home, d, n_d) + others(s, seq, n_d)
    meets = meets + jnp.where(lead, half - 1, 1)
    gate_copy.wait()
    for c in range(0, HEADS * VDIM, 2 * VDIM):
        at = slice(c, c + 2 * VDIM)
        g = gate_v[:, at].astype(jnp.float32)
        gated_ref[:, at] = g / (1.0 + jnp.exp(-g))
    pl.semaphore_wait(barrier, meets)

    first_sends = []
    for ch in range(CHUNKS):
        at = pl.ds(ch * chunk, chunk)
        for k in range(groups):
            to = ((2 * k + core) * half + y, d)
            first_sends.append(
                (lat_ref.at[at], latz.at[z, at], lat_send.at[k, ch], lat_mid.at[z, ch], *to)
            )
            if ch == 0:
                first_sends.append((rk_ref, rkz.at[z], rk_send.at[k], rk_mid.at[z], *to))

    def forwards(from_z, ch):
        slot = from_z * half + y
        at = pl.ds(ch * chunk, chunk)
        for k in range(half):
            to = (z * half + host_y, 2 * k + 1 - zl)
            yield (
                latz.at[from_z, at], latb.at[slot, at], lat_fwd.at[from_z, k, ch],
                lat_recv.at[slot], *to,
            )
            if ch == 0:
                yield rkz.at[from_z], rkb.at[slot], rk_fwd.at[from_z, k], rk_recv.at[slot], *to

    def relays(slot):
        to = {"sp": s, "dp": partner}
        for buf, ssem, rsem in ((latb, relay_lat, lat_recv), (rkb, relay_rk, rk_recv)):
            yield pltpu.make_async_remote_copy(
                buf.at[slot], buf.at[slot], ssem.at[slot], rsem.at[slot],
                device_id=to, device_id_type=MESH,
            )

    def query_sends_of(p):
        for t in TARGETS:
            t = ((x + t // 2) % half) * 2 + (core + t % 2) % 2
            yield (
                q_ref.at[:, pl.ds(pl.multiple_of((t * pairs + p) * PAIR, PAIR), PAIR)],
                qb.at[m, p], q_send.at[t, p], q_recv.at[m, p], zh * n_d + home, t,
            )

    query_sends = [args for p in range(pairs) for args in query_sends_of(p)]

    for copy in small_copies[:2]:
        copy.wait()
    for args in first_sends:
        send(*args)

    def query_part(p):
        for args in query_sends[p * n_d : (p + 1) * n_d]:
            send(*args)

    @pl.when(jnp.logical_not(lead))
    def _():
        for p in range(pairs):
            if CROSSING_AT[p % len(CROSSING_AT)] == 0:
                query_part(p)

    lane = lax.broadcasted_iota(jnp.int32, (rows, 128), 1)
    mask = (lane % 64) < 32
    sign = jnp.where(mask, -1.0, 1.0).astype(jnp.float32)
    low = lax.broadcasted_iota(jnp.int32, (half * rows, 128), 1) < 64

    def tables(block):
        ca, sa = ta_ref[0], ta_ref[1]
        cb, sb = tb_ref[0, block], tb_ref[1, block]
        return ca * cb - sa * sb, (sa * cb + ca * sb) * sign

    def nearest(here, i, count):
        if count & (count - 1):
            return (here + i) % count
        out, bit = 0, 1
        while bit < count:
            out = out + bit * ((here // bit + i // bit) % 2)
            bit *= 2
        return out

    w_copy.wait()
    for copy in small_copies[2:]:
        copy.wait()

    stages = [[(i, ch) for i in range(2) for ch in range(CHUNKS)]]
    stages += [[(i, ch) for i in range(2, n_z)] for ch in range(CHUNKS)]
    starts = [sum(map(len, stages[:k])) for k in range(len(stages) + 1)]

    def forward_stage(k):
        for n, (i, ch) in enumerate(stages[k], starts[k]):
            for p in range(pairs):
                if QUERIES_AT[p % len(QUERIES_AT)] == n:
                    query_part(p)
            from_z = nearest(z, i, n_z)
            at = pl.ds(ch * chunk, chunk)
            arrived(latz.at[from_z, at], lat_mid.at[from_z, ch])
            if ch == 0:
                arrived(rkz.at[from_z], rk_mid.at[from_z])
            for args in forwards(from_z, ch):
                away(*args).start()
        if k == len(stages) - 1:
            for p in range(pairs):
                if QUERIES_AT[p % len(QUERIES_AT)] >= starts[-1]:
                    query_part(p)

    def key_step(i, carry):
        for k in range(len(stages)):

            @pl.when(lead & (i == k))
            def _():
                forward_stage(k)

        from_z = nearest(z, i, n_z)
        for k in range(half):
            slot = from_z * half + k
            here = slice(k * rows, (k + 1) * rows)
            arrived(latb.at[slot], lat_recv.at[slot])
            arrived(rkb.at[slot], rk_recv.at[slot])

            @pl.when(jnp.logical_not(lead))
            def _():
                for copy in relays(slot):
                    copy.start()

            wide = latb[slot].astype(jnp.float32)
            scale = lax.rsqrt(jnp.mean(wide * wide, axis=-1, keepdims=True) + EPS)
            normed[here, :] = (wide * scale * lgain_ref[...]).astype(jnp.bfloat16)
            cosine, sine = tables(slot)
            raw = rkb[slot].astype(jnp.float32).T
            rot[here, :] = turn(
                jnp.concatenate([raw, jnp.zeros_like(raw)], axis=1), cosine, sine, mask
            )
        at = pl.ds(pl.multiple_of(from_z * half * rows, half * rows), half * rows)
        for h in range(heads):
            both = jnp.dot(
                normed[...], w_v[:, h * 256 : (h + 1) * 256], preferred_element_type=jnp.float32
            )
            plain = both[:, :NOPE]
            if h % 2 == 0:
                first, second = plain, rot[...]
            else:
                moved = pltpu.roll(plain, 64, 1)
                first = jnp.where(low, 0.0, moved)
                second = jnp.where(low, moved, pltpu.roll(rot[...], 64, 1))
            kbuf[h, at, :128] = first.astype(jnp.bfloat16)
            kbuf[h, at, 128:] = second.astype(jnp.bfloat16)
            vbuf[h, at, :VDIM] = both[:, NOPE:].astype(jnp.bfloat16)
            vbuf[h, at, VDIM:] = jnp.ones((half * rows, 128), jnp.bfloat16)
        for step in sorted(set(CROSSING_AT) - {0}):

            @pl.when(jnp.logical_not(lead) & (i + 1 == step))
            def _():
                for p in range(pairs):
                    if CROSSING_AT[p % len(CROSSING_AT)] == step:
                        query_part(p)
        return carry

    lax.fori_loop(0, n_z, key_step, 0)

    factor = LOG2E * QDIM ** -0.5

    def output_send(j, p):
        return (ob.at[j, p], orecv.at[d, p], o_send.at[j, p], o_recv.at[d, p], zh * n_d + j, seq)

    def query_step(p, carry):
        for slot in range(n_d):
            arrived(qb.at[slot, p], q_recv.at[slot, p])
            cosine, sine = tables(zh * n_d + slot)
            cosine_high, sine_high = pltpu.roll(cosine, 64, 1), pltpu.roll(sine, 64, 1)
            here = slice(slot * rows, (slot + 1) * rows)
            rq[here, :128] = qb[slot, p, :, :128]
            v = qb[slot, p, :, 128:256].astype(jnp.float32)
            rq[here, 128:256] = turn(v, cosine, sine, mask).astype(jnp.bfloat16)
            v = qb[slot, p, :, 256:].astype(jnp.float32)
            rq[here, 256:] = turn(v, cosine_high, sine_high, mask).astype(jnp.bfloat16)
        for odd in range(2):
            h = 2 * p + odd
            scores = lax.dot_general(
                rq[:, odd * 128 : odd * 128 + KDIM], kbuf[h], DN_T, preferred_element_type=jnp.float32
            )
            top = jnp.max(scores, axis=-1, keepdims=True)
            raised = jnp.exp2((scores - top) * factor).astype(jnp.bfloat16)
            total = jnp.dot(raised, vbuf[h], preferred_element_type=jnp.float32)
            result = (total[:, :VDIM] / total[:, VDIM:]).astype(jnp.bfloat16)
            at = slice(odd * VDIM, (odd + 1) * VDIM)
            for slot in range(n_d):
                ob[slot, p, :, at] = result[slot * rows : (slot + 1) * rows]
        for slot in range(n_d):
            send(*output_send(slot, p))
        return carry

    lax.fori_loop(0, pairs, query_step, 0)

    square = jnp.zeros((rows, 1), jnp.float32)
    for p in range(pairs):
        for t in range(n_d):
            c = (t * pairs + p) * 2 * VDIM
            at = slice(c, c + 2 * VDIM)
            arrived(orecv.at[t, p], o_recv.at[t, p])
            gated = orecv[t, p].astype(jnp.float32) * gated_ref[:, at]
            gated_ref[:, at] = gated
            square = square + jnp.sum(gated * gated, axis=-1, keepdims=True)
    scale = lax.rsqrt(square / (HEADS * VDIM) + EPS)
    scale_ref[...] = jnp.broadcast_to(scale, scale_ref.shape)

    for args in first_sends + query_sends:
        sent(*args)

    @pl.when(lead)
    def _():
        for i in range(n_z):
            for ch in range(CHUNKS):
                for args in forwards(i, ch):
                    away(*args).wait_send()

    @pl.when(jnp.logical_not(lead))
    def _():
        def relayed(i, carry):
            for copy in relays(i):
                copy.wait_send()
            return carry

        lax.fori_loop(0, n_s, relayed, 0)

    def output_sent(i, carry):
        sent(*output_send(i // pairs, i % pairs))
        return carry

    lax.fori_loop(0, n_d * pairs, output_sent, 0)


def angle_tables(rows, n_s):
    half = ROPE // 2
    inverse = np.zeros(128)
    inverse[:ROPE] = np.tile(THETA ** (-np.arange(half) / half), 2)
    inner = np.arange(rows)[:, None] * inverse[None, :]
    outer = (np.arange(n_s) * rows)[:, None] * inverse[None, :]
    inner = np.stack([np.cos(inner), np.sin(inner)]).astype(np.float32)
    outer = np.stack([np.cos(outer), np.sin(outer)]).astype(np.float32)
    return jnp.asarray(inner), jnp.asarray(outer[:, :, None, :])


def per_device(n_s, n_d, queries, latent, rope_key, latent_gain, kv_weight, gate, out_gain):
    rows, rank = latent.shape
    heads = HEADS // n_d
    pairs = heads // 2
    seq = rows * n_s
    inner, outer = angle_tables(rows, n_s)
    bf = jnp.bfloat16
    dma = pltpu.SemaphoreType.DMA
    vmem = pl.BlockSpec(memory_space=pltpu.VMEM)
    hbm = pl.BlockSpec(memory_space=pl.ANY)
    half = n_d // 2
    n_z = n_s // half
    gated, scale = pl.pallas_call(
        functools.partial(kernel, n_s, n_d),
        out_shape=(
            pltpu.VMEM(gate.shape, jnp.float32),
            pltpu.VMEM((rows, 128), jnp.float32),
        ),
        in_specs=[hbm] * 8,
        out_specs=(vmem, vmem),
        scratch_shapes=[
            pltpu.VMEM(kv_weight.shape, bf),
            pltpu.VMEM(gate.shape, bf),
            pltpu.VMEM(latent.shape, bf),
            pltpu.VMEM((ROPE, rows), bf),
            pltpu.VMEM((1, rank), jnp.float32),
            pltpu.VMEM(inner.shape, jnp.float32),
            pltpu.VMEM(outer.shape, jnp.float32),
            pltpu.VMEM((n_z, rows, rank), bf),
            pltpu.VMEM((n_z, ROPE, rows), bf),
            pltpu.VMEM((n_s, rows, rank), bf),
            pltpu.VMEM((n_s, ROPE, rows), bf),
            pltpu.VMEM((half * rows, rank), bf),
            pltpu.VMEM((half * rows, 128), jnp.float32),
            pltpu.VMEM((n_d, pairs, rows, PAIR), bf),
            pltpu.VMEM((heads, seq, KDIM), bf),
            pltpu.VMEM((heads, seq, 2 * VDIM), bf),
            pltpu.VMEM((n_d * rows, PAIR), bf),
            pltpu.VMEM((n_d, pairs, rows, 2 * VDIM), bf),
            pltpu.VMEM((n_d, pairs, rows, 2 * VDIM), bf),
            dma, dma, dma((5,)),
            dma((n_z // 2, CHUNKS)), dma((n_z, CHUNKS)), dma((n_z // 2,)), dma((n_z,)),
            dma((n_z, half, CHUNKS)), dma((n_z, half)),
            *[dma((n_s,))] * 4,
            *[dma((n_d, pairs))] * 4,
        ],
        compiler_params=pltpu.CompilerParams(
            collective_id=0, has_side_effects=True, vmem_limit_bytes=60 * 1024 * 1024
        ),
        name="latent_attention",
    )(
        queries, latent, rope_key.T, latent_gain[None, :], kv_weight, gate, inner, outer,
    )
    return (gated * scale[:, :1] * out_gain[None, :]).astype(bf)


def solution(mesh):
    return jax.shard_map(
        functools.partial(per_device, mesh.shape["sp"], mesh.shape["dp"]),
        mesh=mesh,
        in_specs=(
            P(("dp", "sp"), None),
            P(("dp", "sp"), None),
            P(("dp", "sp"), None),
            P(),
            P(None, "dp"),
            P(("dp", "sp"), None),
            P(),
        ),
        out_specs=P(("dp", "sp"), None),
        check_vma=False,
    )
```
